32 devices in a mesh: fs: 8 (over z, x), tp: 4 (over y, core).
Axes of the slice: x: 2, y: 2, z: 4, core: 2. Of those that a mesh axis runs over, the one named last changes fastest.
Arguments:
- tokens: bfloat16 [16, 384, 2048], P('fs', None, 'tp'), may hold values from -20 to 20
- first_gain: float32 [2048], replicated, may hold values from 0.1 to 1.9
- first_gate: bfloat16 [2048, 5120], P('fs', 'tp'), may hold values from -0.125 to 0.125
- first_up: bfloat16 [2048, 5120], P('fs', 'tp'), may hold values from -0.125 to 0.125
- first_down: bfloat16 [5120, 2048], P('tp', 'fs'), may hold values from -0.078125 to 0.078125
- mixer_gain: float32 [2048], replicated, may hold values from 0.1 to 1.9
- conv_input: bfloat16 [2048, 1024], P('fs', 'tp'), may hold values from -0.125 to 0.125
- outer_gate: bfloat16 [2048, 1024], P('fs', 'tp'), may hold values from -0.125 to 0.125
- inner_gate: bfloat16 [2048, 1024], P('fs', 'tp'), may hold values from -0.125 to 0.125
- conv_taps: float32 [3, 1024], P(None, 'tp'), may hold values from -3.5 to 3.5
- mixer_out: bfloat16 [1024, 2048], P('tp', 'fs'), may hold values from -0.1875 to 0.1875
- second_gain: float32 [2048], replicated, may hold values from 0.1 to 1.9
- second_gate: bfloat16 [2048, 5120], P('fs', 'tp'), may hold values from -0.125 to 0.125
- second_up: bfloat16 [2048, 5120], P('fs', 'tp'), may hold values from -0.125 to 0.125
- second_down: bfloat16 [5120, 2048], P('tp', 'fs'), may hold values from -0.078125 to 0.078125
Outputs:
- layer_out: bfloat16 [16, 384, 2048], P('fs', None, 'tp')
The draws below stay inside these ranges and needn't reach their ends.
All inputs are finite; a program needn't handle non-finite values.
Results may differ from the reference program's by a relative error of at most 0.015.
Values may be sent and summed in bfloat16 or wider, within the bound.
No kernel may reach another device: no remote copies, remote signals or barrier semaphores. Data moves between devices by JAX's collectives and lax.ppermute only.
A program may use at most 64 MiB of HBM per device.

```python
import jax
import jax.numpy as jnp
from jax import lax

D = 2048
FF = 5120
CW = 1024
KERNEL = 3
LEN = 384
SEQS = 16
N_TP = 4


def draw_tokens(key, part):
    key_base, key_block, key_scale = jax.random.split(key, 3)
    blocks = jax.random.uniform(key_block, (SEQS, LEN, N_TP, 1), jnp.float32, -1.1, 1.1)
    base = jnp.clip(jax.random.normal(key_base, (SEQS, LEN, N_TP, D // N_TP), jnp.float32), -6.0, 6.0)
    return (base * jnp.exp(blocks)).reshape(SEQS, LEN, D).astype(jnp.bfloat16)


def block_scale(key, extent, cuts, low, top_value):
    loudness = 1.0
    for axis_at, shards_of in cuts:
        draws = jax.random.uniform(jax.random.fold_in(jax.random.fold_in(key, 6), axis_at), (shards_of,), jnp.float32, low / len(cuts), top_value / len(cuts))
        loudness = loudness * jnp.repeat(jnp.exp(draws), extent[axis_at] // shards_of).reshape((-1,) + (1,) * (len(extent) - 1 - axis_at))
    return loudness


def normal_values(stream_key, dims, scale, bound, shards=(), held_as=jnp.bfloat16):
    result = jax.random.normal(stream_key, dims, jnp.float32) * scale
    if len(shards) > 0:
        result = block_scale(stream_key, dims, shards, -0.22, 0.18) * result
    return jnp.clip(result, min=-bound, max=bound).astype(held_as)


def setup_inputs(seed: int = 0) -> dict:
    keys = jax.random.split(jax.random.key(seed), 16)
    return {
        "tokens": draw_tokens(jax.random.fold_in(keys[15], 71), 0),
        "first_gain": jnp.clip(1.0 + 0.18 * jax.random.normal(keys[1], (D,), jnp.float32), 0.1, 1.9),
        "first_gate": normal_values(keys[2], (D, FF), D ** -0.5, 0.125, ((0, 8), (1, 4))),
        "first_up": normal_values(keys[3], (D, FF), D ** -0.5, 0.125, ((0, 8), (1, 4))),
        "first_down": normal_values(keys[4], (FF, D), FF ** -0.5, 0.078125, ((0, 4), (1, 8))),
        "mixer_gain": jnp.clip(1.0 + 0.18 * jax.random.normal(keys[5], (D,), jnp.float32), 0.1, 1.9),
        "conv_input": normal_values(keys[6], (D, CW), D ** -0.5, 0.125, ((0, 8), (1, 4))),
        "outer_gate": normal_values(keys[7], (D, CW), D ** -0.5, 0.125, ((0, 8), (1, 4))),
        "inner_gate": normal_values(keys[8], (D, CW), D ** -0.5, 0.125, ((0, 8), (1, 4))),
        "conv_taps": normal_values(keys[9], (KERNEL, CW), KERNEL ** -0.5, 3.5, ((1, 4),), jnp.float32),
        "mixer_out": normal_values(keys[10], (CW, D), CW ** -0.5, 0.1875, ((0, 4), (1, 8))),
        "second_gain": jnp.clip(1.0 + 0.18 * jax.random.normal(keys[11], (D,), jnp.float32), 0.1, 1.9),
        "second_gate": normal_values(keys[12], (D, FF), D ** -0.5, 0.125, ((0, 8), (1, 4))),
        "second_up": normal_values(keys[13], (D, FF), D ** -0.5, 0.125, ((0, 8), (1, 4))),
        "second_down": normal_values(keys[14], (FF, D), FF ** -0.5, 0.078125, ((0, 4), (1, 8))),
    }


epsilon = 1e-05

def norm_rows(stream, gain):
    values = stream.astype(jnp.float32)
    scale = lax.rsqrt(lax.optimization_barrier(jnp.mean(values * values, axis=1, keepdims=True)) + epsilon)
    return (values * scale * gain).astype(jnp.bfloat16)

def block_sum(hidden, weight):
    count, inner = hidden.shape
    width = inner // N_TP
    hidden_blocks = hidden.reshape(count, N_TP, width).transpose(1, 0, 2)
    weight_blocks = weight.reshape(N_TP, width, weight.shape[1])

    def add_block(total, pair):
        part = jnp.dot(pair[0], pair[1], preferred_element_type=jnp.float32).astype(jnp.bfloat16)
        part = lax.optimization_barrier(part)
        return (total + part.astype(jnp.float32), None)
    start = jnp.zeros((count, weight.shape[1]), jnp.float32)
    total, _ = lax.scan(add_block, start, (hidden_blocks, weight_blocks))
    return total

def half_ffn(stream, gain, gate_weight, up_weight, down_weight):
    normed = norm_rows(stream, gain)
    gate = jnp.dot(normed, gate_weight, preferred_element_type=jnp.float32)
    upward = jnp.dot(normed, up_weight, preferred_element_type=jnp.float32)
    hidden = (jax.nn.silu(gate) * upward).astype(jnp.bfloat16)
    branch = block_sum(hidden, down_weight)
    return (stream.astype(jnp.float32) + 0.5 * branch).astype(jnp.bfloat16)

def conv_mixer(stream, seqs, gain, conv_input, outer_gate, inner_gate, conv_taps, mixer_out):
    normed = norm_rows(stream, gain)
    conv_values = jnp.dot(normed, conv_input, preferred_element_type=jnp.float32)
    outer = jnp.dot(normed, outer_gate, preferred_element_type=jnp.float32)
    inner = jnp.dot(normed, inner_gate, preferred_element_type=jnp.float32)
    gated_input = (inner * conv_values).reshape(seqs, -1, conv_values.shape[1])
    one_back = jnp.pad(gated_input, ((0, 0), (1, 0), (0, 0)))[:, :-1]
    two_back = jnp.pad(gated_input, ((0, 0), (2, 0), (0, 0)))[:, :-2]
    convolved = conv_taps[0] * two_back + conv_taps[1] * one_back + conv_taps[2] * gated_input
    mixed = (outer * convolved.reshape(conv_values.shape)).astype(jnp.bfloat16)
    branch = block_sum(mixed, mixer_out)
    return (stream.astype(jnp.float32) + branch).astype(jnp.bfloat16)

def reference(tokens, first_gain, first_gate, first_up, first_down, mixer_gain, conv_input, outer_gate, inner_gate, conv_taps, mixer_out, second_gain, second_gate, second_up, second_down):
    seqs, length, width = tokens.shape
    stream = tokens.reshape(seqs * length, width)
    stream = half_ffn(stream, first_gain, first_gate, first_up, first_down)
    stream = conv_mixer(stream, seqs, mixer_gain, conv_input, outer_gate, inner_gate, conv_taps, mixer_out)
    stream = half_ffn(stream, second_gain, second_gate, second_up, second_down)
    return stream.reshape(seqs, length, width)
```

```python
import math

import jax
import jax.numpy as jnp
from jax import lax
from jax.sharding import PartitionSpec as P

epsilon = 1e-05


def line_ring(count):
    return [0] + list(range(1, count, 2)) + [k for k in range(count - 1, 0, -1) if k % 2 == 0]


class Layout:
    def __init__(self, mesh):
        self.fs = mesh.shape["fs"]
        self.tp = mesh.shape["tp"]
        self.nx = max(k for k in range(1, math.isqrt(self.fs) + 1) if self.fs % k == 0)
        self.nz = self.fs // self.nx
        self.cores = 2 if self.tp % 2 == 0 else 1
        self.ny = self.tp // self.cores
        self.z_ring = line_ring(self.nz)
        self.x_ring = line_ring(self.nx)

    def z_step(self, array):
        nxt = {a: b for a, b in zip(self.z_ring, self.z_ring[1:] + self.z_ring[:1])}
        return lax.ppermute(
            array, "fs", [(z * self.nx + x, nxt[z] * self.nx + x) for z in range(self.nz) for x in range(self.nx)]
        )

    def x_step(self, array):
        nxt = {a: b for a, b in zip(self.x_ring, self.x_ring[1:] + self.x_ring[:1])}
        return lax.ppermute(
            array, "fs", [(z * self.nx + x, z * self.nx + nxt[x]) for z in range(self.nz) for x in range(self.nx)]
        )

    def core_step(self, array):
        n = self.cores
        return lax.ppermute(array, "tp", [(t, t // n * n + (t % n + 1) % n) for t in range(self.tp)])

    def y_step(self, array, shift):
        n = self.cores
        return lax.ppermute(array, "tp", [(t, (t // n + shift) % self.ny * n + t % n) for t in range(self.tp)])

    def place(self, zs, xs):
        at = lax.axis_index("fs")
        zr, xr = self.z_ring, self.x_ring
        table = []
        for k in range(self.fs):
            z, x = k // self.nx, k % self.nx
            table.append(zr[(zr.index(z) - zs) % self.nz] * self.nx + xr[(xr.index(x) - xs) % self.nx])
        return jnp.array(table, jnp.int32)[at]


def halves(block):
    return block.reshape(2, block.shape[0] // 2, block.shape[1])


def stream(lay, blocks, gate_on=None):
    if gate_on is not None:
        blocks, _ = lax.optimization_barrier((blocks, gate_on))
    count = len(blocks)
    slots = [[] for _ in blocks]
    split = lay.nx == 2 and lay.nz > 2
    along_z = [list(blocks)]
    along_x = [[b] for b in blocks]
    for k in range(count):
        slots[k].append((blocks[k], 0, 0, None))
    first_swapped = [lay.x_step(b) for b in blocks]
    for step in range(1, lay.nz):
        along_z.append([lay.z_step(b) for b in along_z[-1]])
    for step in range(lay.nz):
        for k in range(count):
            block = along_z[step][k]
            if step:
                slots[k].append((block, step, 0, None))
            if step == 1 and split:
                low, high = halves(block)
                slots[k].append((lay.x_step(high), step, 1, 1))
                slots[k].append((lay.z_step(halves(first_swapped[k])[0]), step, 1, 0))
                continue
            moved = block
            for hop in range(1, lay.nx):
                moved = first_swapped[k] if step == 0 and hop == 1 else lay.x_step(moved)
                slots[k].append((moved, step, hop, None))
    wholes = []
    for k in range(count):
        rows, cols = blocks[k].shape
        whole = jnp.zeros((lay.fs, 2, rows // 2, cols), blocks[k].dtype)
        for block, zs, xs, half in slots[k]:
            at = lay.place(zs, xs)
            if half is None:
                whole = lax.dynamic_update_slice(whole, halves(block)[None], (at, 0, 0, 0))
            else:
                whole = lax.dynamic_update_slice(whole, block[None, None], (at, half, 0, 0))
        wholes.append(whole.reshape(lay.fs, rows, cols))
    return wholes, along_z[min(2, lay.nz - 1)]


def gather_rows(lay, stream_rows):
    tp = lay.tp
    pieces = [stream_rows]
    for shift in range(1, lay.ny):
        pieces.append(lay.y_step(stream_rows, shift))
    if lay.cores == 2:
        pieces = pieces + [lay.core_step(p) for p in pieces]
    at = lax.axis_index("tp")
    y, c = at // lay.cores, at % lay.cores
    stack = jnp.stack(pieces)
    ordered = []
    for t in range(tp):
        ty, tc = t // lay.cores, t % lay.cores
        shift = (y - ty) % lay.ny
        other = (tc != c).astype(jnp.int32)
        ordered.append(lax.dynamic_index_in_dim(stack, other * lay.ny + shift, 0, keepdims=False))
    return jnp.concatenate(ordered, axis=1)


def norm_rows(lay, stream_rows, gain):
    values = gather_rows(lay, stream_rows).astype(jnp.float32)
    scale = lax.rsqrt(jnp.mean(values * values, axis=1, keepdims=True) + epsilon)
    return (values * scale * gain).astype(jnp.bfloat16)


def dot(a, b):
    return jnp.dot(a, b, preferred_element_type=jnp.float32)


def scatter_columns(lay, hidden, whole):
    rows = hidden.shape[0]
    per = lay.fs // lay.tp
    parts = jnp.stack([dot(hidden, whole[b]).astype(jnp.bfloat16) for b in range(lay.fs)])
    cols = parts.shape[2]
    parts = parts.reshape(lay.ny, lay.cores, per * rows, cols)
    at = lax.axis_index("tp")
    y, c = at // lay.cores, at % lay.cores
    keep = lax.dynamic_index_in_dim(parts, c, 1, keepdims=False).astype(jnp.float32)
    if lay.cores == 2:
        send = lax.dynamic_index_in_dim(parts, 1 - c, 1, keepdims=False)
        keep = keep + lay.core_step(send).astype(jnp.float32)
    total = lax.dynamic_index_in_dim(keep, y, 0, keepdims=False)
    for shift in range(1, lay.ny):
        piece = lax.dynamic_index_in_dim(keep, (y + shift) % lay.ny, 0, keepdims=False).astype(jnp.bfloat16)
        total = total + lay.y_step(piece, shift).astype(jnp.float32)
    return total.reshape(per, rows, cols).transpose(1, 0, 2).reshape(rows, per * cols)


def ffn_hidden(normed, gate, up):
    gate = dot(normed, gate.reshape(-1, gate.shape[2]))
    up = dot(normed, up.reshape(-1, up.shape[2]))
    return (jax.nn.silu(gate) * up).astype(jnp.bfloat16)


def mix(normed, whole, conv_taps, seqs):
    made = dot(normed, whole.reshape(-1, whole.shape[2]))
    width = made.shape[1] // 3
    conv_values, outer, inner = made[:, :width], made[:, width : 2 * width], made[:, 2 * width :]
    gated_input = (inner * conv_values).reshape(seqs, -1, width)
    one_back = jnp.pad(gated_input, ((0, 0), (1, 0), (0, 0)))[:, :-1]
    two_back = jnp.pad(gated_input, ((0, 0), (2, 0), (0, 0)))[:, :-2]
    convolved = conv_taps[0] * two_back + conv_taps[1] * one_back + conv_taps[2] * gated_input
    return (outer * convolved.reshape(outer.shape)).astype(jnp.bfloat16)


def add_branch(stream_rows, branch):
    return (stream_rows.astype(jnp.float32) + branch).astype(jnp.bfloat16)


def solution(mesh):
    lay = Layout(mesh)

    def on_device(
        tokens, first_gain, first_gate, first_up, first_down, mixer_gain, conv_input, outer_gate, inner_gate,
        conv_taps, mixer_out, second_gain, second_gate, second_up, second_down,
    ):
        seqs, length, width = tokens.shape
        rows = tokens.reshape(seqs * length, width)
        mixer_in = jnp.concatenate([conv_input, outer_gate, inner_gate], axis=1)
        (fg, fu), mark = stream(lay, [first_gate, first_up])
        (fd, mi, mo), mark = stream(lay, [first_down, mixer_in, mixer_out], mark)
        (sg, su), mark = stream(lay, [second_gate, second_up], mark)
        (sd,), mark = stream(lay, [second_down], mark)

        hidden = ffn_hidden(norm_rows(lay, rows, first_gain), fg, fu)
        rows = add_branch(rows, 0.5 * scatter_columns(lay, hidden, fd))
        mixed = mix(norm_rows(lay, rows, mixer_gain), mi, conv_taps, seqs)
        rows = add_branch(rows, scatter_columns(lay, mixed, mo))
        hidden = ffn_hidden(norm_rows(lay, rows, second_gain), sg, su)
        rows = add_branch(rows, 0.5 * scatter_columns(lay, hidden, sd))
        return rows.reshape(seqs, length, width)

    in_specs = (
        P("fs", None, "tp"), P(), P("fs", "tp"), P("fs", "tp"), P("tp", "fs"), P(), P("fs", "tp"), P("fs", "tp"),
        P("fs", "tp"), P(None, "tp"), P("tp", "fs"), P(), P("fs", "tp"), P("fs", "tp"), P("tp", "fs"),
    )
    return jax.shard_map(on_device, mesh=mesh, in_specs=in_specs, out_specs=P("fs", None, "tp"), check_vma=False)
```
